32 devices in a mesh: ep: 8 (over z, y), tp: 4 (over x, core).
Axes of the slice: x: 2, y: 2, z: 4, core: 2. Of those that a mesh axis runs over, the one named last changes fastest.
Arguments:
- mixer_input_rows: bfloat16 [4096, 2048], P(('ep', 'tp')), may hold values from -6 to 6
- mixer_norm_scale: float32 [2048], replicated, may hold values from 0.1 to 1.9
- decay_bias_table: float32 [4096, 16], P('ep', 'tp'), may hold values from -14 to 1
- erase_bias_table: float32 [16], P('tp'), may hold values from -12 to 1
- receive_weight: bfloat16 [2048, 1024], P(None, 'tp'), may hold values from -0.125 to 0.125
- key_weight: bfloat16 [2048, 1024], P(None, 'tp'), may hold values from -0.125 to 0.125
- value_weight: bfloat16 [2048, 1024], P(None, 'tp'), may hold values from -0.125 to 0.125
- decay_weight: bfloat16 [2048, 1024], P(None, 'tp'), may hold values from -0.125 to 0.125
- erase_weight: bfloat16 [2048, 1024], P(None, 'tp'), may hold values from -0.125 to 0.125
- self_token_scale: float32 [16, 64], P('tp'), may hold values from -0.6 to 0.6
- head_norm_scale: float32 [1024], P('tp'), may hold values from 0.1 to 1.9
- output_weight: bfloat16 [1024, 2048], P('tp'), may hold values from -0.1875 to 0.1875
- expert_input_rows: bfloat16 [4096, 2048], P(('ep', 'tp')), may hold values from -6 to 6
- expert_norm_scale: float32 [2048], replicated, may hold values from 0.1 to 1.9
- routes: int32 [4096, 2], P(('ep', 'tp')), may hold values from 0 to 31, all different within a row; in each aligned block of 128 rows (0 to 127, 128 to 255, ...) at most 16 rows name the same one
- router_weights: float32 [4096, 2], P(('ep', 'tp')), may hold values from 0.1 to 1
- routed_gate_weight: bfloat16 [32, 2048, 1024], P(('ep', 'tp')), may hold values from -0.125 to 0.125
- routed_up_weight: bfloat16 [32, 2048, 1024], P(('ep', 'tp')), may hold values from -0.125 to 0.125
- routed_down_weight: bfloat16 [32, 1024, 2048], P(('ep', 'tp')), may hold values from -0.1875 to 0.1875
- common_gate_weight: bfloat16 [2048, 256], replicated, may hold values from -0.125 to 0.125
- common_up_weight: bfloat16 [2048, 256], replicated, may hold values from -0.125 to 0.125
- common_down_weight: bfloat16 [256, 2048], replicated, may hold values from -0.375 to 0.375
Outputs:
- mixer_output: bfloat16 [4096, 2048], P(('ep', 'tp'))
- mixed_b: bfloat16 [4096, 2048], P(('ep', 'tp'))
The draws below stay inside these ranges and needn't reach their ends.
Inputs may be any that keep to these rules, and one draw needn't show every extreme that they name: `routes`: within the rows of one device no expert is named by more than 16 rows, a bound that some block reaches; each row names 2 different experts, and every expert is named somewhere.
All inputs are finite; a program needn't handle non-finite values.
Results may differ from the reference program's by a relative error of at most 0.015.
Values may be sent and summed in bfloat16 or wider, within the bound.
A program may use at most 128 MiB of HBM per device.

```python
import math
import jax
import jax.numpy as jnp
import numpy as np
from jax import lax

D = 2048
MIXER_HEADS = 16
HEAD_CHANNELS = 64
MIX = 1024
EXPERT_FF = 1024
SHARED_FF = 256
TOPK = 2
TOK_DEV = 128
SEQ_DEV = 512
BATCH_TOKENS = 4096
EXPERTS = 32
CAP = 16
N_TP = 4


def head_speeds(key):
    shuffled = jax.random.permutation(jax.random.fold_in(key, 4101), MIXER_HEADS)
    fast_count = MIXER_HEADS // 2
    return shuffled < fast_count


def draw_mixer_input_rows(key, part):
    block_total = BATCH_TOKENS // 64
    order_key, direction_key, noise_key = jax.random.split(jax.random.fold_in(key, 4104), 3)
    picked = jax.random.permutation(order_key, block_total) < max(block_total // 8, 1)
    directions = jax.random.normal(direction_key, (block_total, D), jnp.float32)
    noise = jax.random.normal(noise_key, (BATCH_TOKENS, D), jnp.float32)
    aligned_rows = jnp.repeat(picked, 64)
    shared_rows = jnp.repeat(directions, 64, axis=0)
    rows = jnp.where(aligned_rows[:, None], 2.4 * shared_rows + 0.6 * noise, noise)
    return jnp.clip(rows, -6.0, 6.0).astype(jnp.bfloat16)


def draw_decay_bias_table(key, part):
    fast_heads = head_speeds(key)
    tier_random_key, spike_key, head_random_key = jax.random.split(jax.random.fold_in(key, 4102), 3)
    block_level = jax.random.uniform(tier_random_key, (BATCH_TOKENS // SEQ_DEV,), jnp.float32, -0.7, 0.7)
    gradual_tier = jnp.log(0.5 / BATCH_TOKENS) + jnp.repeat(block_level, SEQ_DEV)
    token_position = jnp.arange(BATCH_TOKENS, dtype=jnp.int32)
    spike_groups = jax.random.randint(spike_key, (3,), 0, BATCH_TOKENS)
    spike_rows = jnp.any(token_position[:, None] == spike_groups[None, :], axis=1)
    gradual_rows = jnp.where(spike_rows, 0.4, gradual_tier)
    fast_level = jnp.log(0.02) + 0.5 + jax.random.uniform(head_random_key, (MIXER_HEADS,), jnp.float32, -0.4, 0.4)
    return jnp.where(fast_heads[None, :], fast_level[None, :], gradual_rows[:, None]).astype(jnp.float32)


def draw_erase_bias_table(key, part):
    fast_heads = head_speeds(key)
    spread = jax.random.uniform(jax.random.fold_in(key, 4103), (MIXER_HEADS,), jnp.float32, -0.5, 0.5)
    return jnp.where(fast_heads, 0.75 + 0.5 * spread, jnp.log(16.0 / BATCH_TOKENS) + spread).astype(jnp.float32)


def steps_of(key, extent, shards, least, top_value):
    factor_of, own = 1.0, jax.random.fold_in(key, 6)
    for position, shards_of in shards:
        draws = jnp.exp(jax.random.uniform(jax.random.fold_in(own, position), (shards_of,), jnp.float32, least / len(shards), top_value / len(shards)))
        factor_of = factor_of * jnp.repeat(draws, extent[position] // shards_of).reshape([-1 if axis == position else 1 for axis in range(len(extent))])
    return factor_of


def assign_block(rng, own, number, rows, amount, top, most, lean):
    ranking = jax.random.permutation(rng, amount)
    heavy_load, usual = load_shares(amount, rows * top, most, lean, True), load_shares(amount, rows * top, most, lean, False)
    places = jnp.arange(amount)

    def named(sizes, turn):
        used = int((sizes > 0).sum())
        fixed = max(1, used // 4)
        moved = fixed + (places - fixed + turn * (used - fixed)) % max(1, amount - fixed)
        return jnp.zeros((amount,), jnp.int32).at[ranking[jnp.where(places < fixed, places, moved)]].set(jnp.asarray(sizes, jnp.int32))

    sizes = jnp.where(number % 4 == 0, named(heavy_load, number // 4), named(usual, number - number // 4 - 1))
    mixed = jax.random.permutation(jax.random.fold_in(own, 3), amount)
    source_of, receiver = mixed[0:amount // 2 * 2:2], mixed[1:amount // 2 * 2:2]
    room = jnp.minimum(sizes[source_of] - 1, most - sizes[receiver]) // 2
    room = jnp.where((source_of == ranking[0]) | (receiver == ranking[0]) | (sizes[receiver] == 0), 0, jnp.maximum(room, 0))
    moved = jax.random.randint(jax.random.fold_in(own, 4), (amount // 2,), 0, 1 << 20) % (room + 1)
    sizes = sizes.at[source_of].add(-moved).at[receiver].add(moved)
    labels = jnp.searchsorted(jnp.cumsum(sizes), jnp.arange(rows * top), side="right").astype(jnp.int32)
    listing = labels.reshape(top, rows).T
    listing = listing[jax.random.permutation(jax.random.fold_in(own, 1), rows)]
    turn = jax.random.randint(jax.random.fold_in(own, 2), (rows, 1), 0, top)
    return jnp.take_along_axis(listing, (jnp.arange(top)[None, :] + turn) % top, axis=1)


def load_shares(amount, total, bound, lean, full):
    portions = [(1 << 20) // math.isqrt(standing ** lean) + 1 for standing in range(1, amount + 1)]
    largest = bound if full else min(bound, max(-(-total // amount), total * portions[0] // sum(portions)))
    least = 1 if total - largest >= amount - 1 else 0
    counts, rest = [largest] + [least] * (amount - 1), total - largest - least * (amount - 1)
    while rest > 0:
        free = [i for i in range(1, amount) if counts[i] < largest] or [i for i in range(1, amount) if counts[i] < bound]
        mass, remaining = sum([portions[i] for i in free]), rest
        for i in free:
            addition = min(bound - counts[i], max(1, remaining * portions[i] // mass), rest)
            counts[i] = counts[i] + addition
            rest = rest - addition
    return np.array(counts)


def scatter_about(stream_key, extent, scale, limit, pieces=(), kind=jnp.bfloat16):
    values = scale * jax.random.normal(stream_key, extent, jnp.float32)
    if pieces:
        values = values * steps_of(stream_key, extent, pieces, -0.22, 0.18)
    return jnp.clip(values, -limit, limit).astype(kind)


def setup_inputs(seed: int = 0) -> dict:
    key_of = jax.random.split(jax.random.key(seed), 23)
    mixer_input_rows = draw_mixer_input_rows(jax.random.fold_in(key_of[22], 71), 0)
    mixer_norm_scale = jnp.clip(1.0 + 0.18 * jax.random.normal(key_of[1], (D,), jnp.float32), 0.1, 1.9)
    decay_bias_table = draw_decay_bias_table(jax.random.fold_in(key_of[22], 71), 0)
    erase_bias_table = draw_erase_bias_table(jax.random.fold_in(key_of[22], 71), 0)
    receive_weight = scatter_about(key_of[4], (D, MIX), D ** -0.5, 0.125, ((1, 4),))
    key_weight = scatter_about(key_of[5], (D, MIX), D ** -0.5, 0.125, ((1, 4),))
    value_weight = scatter_about(key_of[6], (D, MIX), D ** -0.5, 0.125, ((1, 4),))
    decay_weight = scatter_about(key_of[7], (D, MIX), D ** -0.5, 0.125, ((1, 4),))
    erase_weight = scatter_about(key_of[8], (D, MIX), D ** -0.5, 0.125, ((1, 4),))
    self_token_scale = scatter_about(key_of[9], (MIXER_HEADS, HEAD_CHANNELS), 0.1, 0.6, ((0, 4),), jnp.float32)
    head_norm_scale = jnp.clip(1.0 + 0.18 * jax.random.normal(key_of[10], (MIX,), jnp.float32), 0.1, 1.9)
    output_weight = scatter_about(key_of[11], (MIX, D), MIX ** -0.5, 0.1875, ((0, 4),))
    expert_input_rows = scatter_about(key_of[12], (BATCH_TOKENS, D), 1.0, 6.0, ((0, 32),))
    expert_norm_scale = jnp.clip(1.0 + 0.18 * jax.random.normal(key_of[13], (D,), jnp.float32), 0.1, 1.9)
    routes_keys = jax.random.split(jax.random.fold_in(key_of[14], 1), BATCH_TOKENS // TOK_DEV)
    routes_turns = jax.random.permutation(jax.random.fold_in(key_of[14], 3), BATCH_TOKENS // TOK_DEV)
    routes = jax.vmap(lambda own, number: assign_block(jax.random.fold_in(key_of[14], 2), own, number, TOK_DEV, EXPERTS, TOPK, CAP, 1))(routes_keys, routes_turns).reshape((BATCH_TOKENS, TOPK))
    router_weights = jnp.clip(jnp.exp(math.log(1.0) - 2.3025851 * jax.random.uniform(key_of[15], (BATCH_TOKENS, TOPK), jnp.float32) ** steps_of(key_of[15], (BATCH_TOKENS, TOPK), ((0, 32),), -0.2, 0.2)), 0.1, 1.0)
    routed_gate_weight = scatter_about(key_of[16], (EXPERTS, D, EXPERT_FF), D ** -0.5, 0.125, ((0, 32),))
    routed_up_weight = scatter_about(key_of[17], (EXPERTS, D, EXPERT_FF), D ** -0.5, 0.125, ((0, 32),))
    routed_down_weight = scatter_about(key_of[18], (EXPERTS, EXPERT_FF, D), EXPERT_FF ** -0.5, 0.1875, ((0, 32),))
    common_gate_weight = scatter_about(key_of[19], (D, SHARED_FF), D ** -0.5, 0.125)
    common_up_weight = scatter_about(key_of[20], (D, SHARED_FF), D ** -0.5, 0.125)
    common_down_weight = scatter_about(key_of[21], (SHARED_FF, D), SHARED_FF ** -0.5, 0.375)
    return dict(mixer_input_rows=mixer_input_rows, mixer_norm_scale=mixer_norm_scale, decay_bias_table=decay_bias_table, erase_bias_table=erase_bias_table, receive_weight=receive_weight, key_weight=key_weight, value_weight=value_weight, decay_weight=decay_weight, erase_weight=erase_weight, self_token_scale=self_token_scale, head_norm_scale=head_norm_scale, output_weight=output_weight, expert_input_rows=expert_input_rows, expert_norm_scale=expert_norm_scale, routes=routes, router_weights=router_weights, routed_gate_weight=routed_gate_weight, routed_up_weight=routed_up_weight, routed_down_weight=routed_down_weight, common_gate_weight=common_gate_weight, common_up_weight=common_up_weight, common_down_weight=common_down_weight)


precise = lax.Precision.HIGHEST

def rms_rows(values, feature_gain):
    wide_values = values.astype(jnp.float32)
    inverse = lax.rsqrt(lax.optimization_barrier(jnp.mean(wide_values * wide_values, axis=-1, keepdims=True)) + 1e-06)
    return (wide_values * inverse * feature_gain).astype(jnp.bfloat16)

def mixer_baseline(mixer_input_rows, mixer_norm_scale, decay_bias_table, erase_bias_table, receive_weight, key_weight, value_weight, decay_weight, erase_weight, self_token_scale, head_norm_scale, output_weight):
    normed_a = rms_rows(mixer_input_rows, mixer_norm_scale)
    token_count = normed_a.shape[0]

    def heads_of(weight_part):
        product = jnp.dot(normed_a, weight_part, preferred_element_type=jnp.float32)
        return product.reshape(token_count, MIXER_HEADS, HEAD_CHANNELS)
    receive_vector = heads_of(receive_weight)
    key_projected = heads_of(key_weight)
    value_projected = heads_of(value_weight)
    log_decay = -jnp.exp(-jax.nn.softplus(-(heads_of(decay_weight) + decay_bias_table[:, :, None])) - 0.5)
    erase_rate = jax.nn.sigmoid(heads_of(erase_weight) + erase_bias_table[None, :, None])
    unit_key = key_projected * lax.rsqrt(lax.optimization_barrier(jnp.sum(key_projected * key_projected, axis=2, keepdims=True)) + 1e-06)

    def advance(state_now, inputs):
        receptance_now, decay_now, key_now, value_now, unit_now, rate_now = inputs
        projected = jnp.einsum('hvk,hk->hv', state_now, unit_now, precision=precise)
        state_now = state_now * jnp.exp(decay_now)[:, None, :] - projected[:, :, None] * (unit_now * rate_now)[:, None, :] + value_now[:, :, None] * key_now[:, None, :]
        return (state_now, jnp.einsum('hvk,hk->hv', state_now, receptance_now, precision=precise))
    start_state = jnp.zeros((MIXER_HEADS, HEAD_CHANNELS, HEAD_CHANNELS), jnp.float32)
    readout = lax.scan(advance, start_state, (receive_vector, log_decay, key_projected, value_projected, unit_key, erase_rate))[1]
    mean_removed = readout - lax.optimization_barrier(jnp.mean(readout, axis=2, keepdims=True))
    squared_mean = lax.optimization_barrier(jnp.mean(mean_removed * mean_removed, axis=2, keepdims=True))
    head_norm_scales = head_norm_scale.reshape(MIXER_HEADS, HEAD_CHANNELS)
    self_token_term = lax.optimization_barrier(jnp.sum(receive_vector * key_projected * self_token_scale[None], axis=2, keepdims=True)) * value_projected
    mixer_head_count = mean_removed * lax.rsqrt(squared_mean + 0.00064) * head_norm_scales + self_token_term
    mixer_head_count = mixer_head_count.reshape(token_count, MIXER_HEADS * HEAD_CHANNELS).astype(jnp.bfloat16)
    group_width = MIXER_HEADS * HEAD_CHANNELS // N_TP
    summed_total = jnp.zeros((token_count, D), jnp.float32)
    for group_index in range(N_TP):
        first_column = group_index * group_width
        partial_sum = jnp.dot(mixer_head_count[:, first_column:first_column + group_width], output_weight[first_column:first_column + group_width], preferred_element_type=jnp.float32).astype(jnp.bfloat16)
        summed_total = summed_total + lax.optimization_barrier(partial_sum).astype(jnp.float32)
    return summed_total.astype(jnp.bfloat16)

def experts_reference(expert_input_rows, expert_norm_scale, routes, router_weights, routed_gate_weight, routed_up_weight, routed_down_weight, common_gate_weight, common_up_weight, common_down_weight):
    normed_b = rms_rows(expert_input_rows, expert_norm_scale)
    route_weight = 2.5 * router_weights / lax.optimization_barrier(jnp.sum(router_weights, axis=1, keepdims=True))
    block_count = BATCH_TOKENS // TOK_DEV
    pair_count = TOK_DEV * TOPK
    chosen = routes.reshape(block_count, pair_count)
    onehot = (chosen[:, :, None] == jnp.arange(EXPERTS, dtype=jnp.int32)[None, None, :]).astype(jnp.int32)
    slot_rank = lax.optimization_barrier(jnp.sum(jnp.cumsum(onehot, axis=1) * onehot, axis=2)) - 1
    slot_index = chosen * CAP + slot_rank
    block_index = jnp.arange(block_count, dtype=jnp.int32)[:, None]
    global_row = block_index * TOK_DEV + (jnp.arange(pair_count, dtype=jnp.int32) // TOPK)[None, :]
    token_table = jnp.zeros((block_count, EXPERTS * CAP), jnp.int32).at[block_index, slot_index].set(global_row)
    weight_table = jnp.zeros((block_count, EXPERTS * CAP), jnp.float32).at[block_index, slot_index].set(route_weight.reshape(block_count, pair_count))
    token_table = token_table.reshape(block_count, EXPERTS, CAP).transpose(1, 0, 2).reshape(EXPERTS, -1)
    weight_table = weight_table.reshape(block_count, EXPERTS, CAP).transpose(1, 0, 2).reshape(EXPERTS, -1)

    def one_expert(running, expert_inputs):
        gate_part, up_part, down_part, token_index, weight_part = expert_inputs
        expert_rows = normed_b[token_index]
        expert_hidden = (jax.nn.silu(jnp.dot(expert_rows, gate_part, preferred_element_type=jnp.float32)) * jnp.dot(expert_rows, up_part, preferred_element_type=jnp.float32)).astype(jnp.bfloat16)
        expert_out = jnp.dot(expert_hidden, down_part, preferred_element_type=jnp.float32).astype(jnp.bfloat16)
        running = running.at[token_index].add(weight_part[:, None] * expert_out.astype(jnp.float32))
        return (running, None)
    routed = lax.scan(one_expert, jnp.zeros((BATCH_TOKENS, D), jnp.float32), (routed_gate_weight, routed_up_weight, routed_down_weight, token_table, weight_table))[0]
    shared_hidden = (jax.nn.silu(jnp.dot(normed_b, common_gate_weight, preferred_element_type=jnp.float32)) * jnp.dot(normed_b, common_up_weight, preferred_element_type=jnp.float32)).astype(jnp.bfloat16)
    shared_term = jnp.dot(shared_hidden, common_down_weight, preferred_element_type=jnp.float32)
    return (routed + shared_term).astype(jnp.bfloat16)

def reference(mixer_input_rows, mixer_norm_scale, decay_bias_table, erase_bias_table, receive_weight, key_weight, value_weight, decay_weight, erase_weight, self_token_scale, head_norm_scale, output_weight, expert_input_rows, expert_norm_scale, routes, router_weights, routed_gate_weight, routed_up_weight, routed_down_weight, common_gate_weight, common_up_weight, common_down_weight):
    mixer_output = mixer_baseline(mixer_input_rows, mixer_norm_scale, decay_bias_table, erase_bias_table, receive_weight, key_weight, value_weight, decay_weight, erase_weight, self_token_scale, head_norm_scale, output_weight)
    mixed_b = experts_reference(expert_input_rows, expert_norm_scale, routes, router_weights, routed_gate_weight, routed_up_weight, routed_down_weight, common_gate_weight, common_up_weight, common_down_weight)
    return (mixer_output, mixed_b)
```

```python
import functools

import jax
import jax.numpy as jnp
from jax import lax
from jax.experimental import pallas as pl
from jax.experimental.pallas import tpu as pltpu
from jax.sharding import PartitionSpec as P

precise = lax.Precision.HIGHEST


def rms_rows(values, feature_gain):
    wide_values = values.astype(jnp.float32)
    inverse = lax.rsqrt(jnp.mean(wide_values * wide_values, axis=1, keepdims=True) + 1e-06)
    return (wide_values * inverse * feature_gain).astype(jnp.bfloat16)


def halves(wide):
    high = wide.astype(jnp.bfloat16)
    return high, (wide - high.astype(jnp.float32)).astype(jnp.bfloat16)


def split_dot(left, right, left_axis, right_axis):
    left_high, left_low = halves(left)
    right_high, right_low = halves(right)
    return lax.dot_general(
        jnp.concatenate([left_high, left_high, left_low], axis=left_axis),
        jnp.concatenate([right_high, right_low, right_high], axis=right_axis),
        (((left_axis,), (right_axis,)), ((), ())),
        preferred_element_type=jnp.float32,
    )


def head_sums(wide, channels):
    rows, width = wide.shape
    same_head = (
        lax.broadcasted_iota(jnp.int32, (width, width), 0) // channels
        == lax.broadcasted_iota(jnp.int32, (width, width), 1) // channels
    )
    ones = jnp.where(same_head, 1.0, 0.0).astype(jnp.bfloat16)
    high, low = halves(wide)
    both = jnp.dot(
        jnp.concatenate([high, low], axis=0), ones, preferred_element_type=jnp.float32
    )
    return both[:rows] + both[rows:]


def scan_kernel(
    channels, block_len, r_ref, k_ref, v_ref, ld_ref, rate_ref, local_ref, through_ref, state_ref, aug_ref
):
    step = pl.program_id(0)
    width = r_ref.shape[1]
    heads = width // channels
    groups = r_ref.shape[0] // block_len

    def iotas(shape):
        return (
            lax.broadcasted_iota(jnp.int32, shape, 0),
            lax.broadcasted_iota(jnp.int32, shape, 1),
        )

    row, col = iotas((block_len, block_len))
    eye = jnp.where(row == col, 1.0, 0.0)
    wide_row, wide_col = iotas((2 * block_len, 2 * block_len))
    local_row, local_col = wide_row % block_len, wide_col % block_len
    keep = (local_row > local_col) | ((local_row == local_col) & (wide_row >= block_len))
    tri_row, tri_col = iotas((block_len, 3 * block_len))
    running = jnp.where(tri_row >= tri_col % block_len, 1.0, 0.0).astype(jnp.bfloat16)

    @pl.when(step == 0)
    def _():
        aug_row, aug_col = iotas((2 * channels, width))
        aug_ref[...] = jnp.where(aug_row - channels == aug_col % channels, 1.0, 0.0)

    pieces = []
    for group in range(groups):
        rows = pl.ds(group * block_len, block_len)
        receive, key, value = r_ref[rows, :], k_ref[rows, :], v_ref[rows, :]
        log_decay, rate = ld_ref[rows, :], rate_ref[rows, :]
        unit = key * lax.rsqrt(head_sums(key * key, channels) + 1e-06)
        high, rest = halves(log_decay)
        middle, low = halves(log_decay - high.astype(jnp.float32))
        cumulative = jnp.dot(
            running,
            jnp.concatenate([high, middle, low], axis=0),
            preferred_element_type=jnp.float32,
        )
        growth = jnp.exp(-cumulative)
        erase_in = -unit * jnp.exp(cumulative - log_decay)
        erase_out = unit * rate * growth
        key_out = key * growth
        read_in = receive * jnp.exp(cumulative)
        last = cumulative[block_len - 1 : block_len, :]
        tail = jnp.exp(last - cumulative)
        erase_tail = unit * rate * tail
        key_tail = key * tail
        total = jnp.exp(last)
        for head in range(heads):
            cut = slice(head * channels, (head + 1) * channels)
            products = split_dot(
                jnp.concatenate([erase_in[:, cut], read_in[:, cut]], axis=0),
                jnp.concatenate([erase_out[:, cut], key_out[:, cut]], axis=0),
                1,
                1,
            )
            products = jnp.where(keep, products, 0.0)
            pieces.append(
                dict(
                    group=group,
                    cut=cut,
                    products=products,
                    erase_in=erase_in[:, cut],
                    read_in=read_in[:, cut],
                    value=value[:, cut],
                    erase_tail=erase_tail[:, cut],
                    key_tail=key_tail[:, cut],
                    total=total[:, cut],
                    erase=products[:block_len, :block_len],
                )
            )
    for piece in pieces:
        piece["inverse"] = eye + jnp.where(row // 2 == col // 2, piece["erase"], 0.0)
    span = 2
    while span < block_len:
        joint = (row // (2 * span) == col // (2 * span)) & (row // span != col // span)
        for piece in pieces:
            piece["half"] = split_dot(piece["inverse"], jnp.where(joint, piece["erase"], 0.0), 1, 0)
        for piece in pieces:
            piece["inverse"] = piece["inverse"] + split_dot(piece["half"], piece["inverse"], 1, 0)
        span *= 2
    for piece in pieces:
        piece["valued"] = split_dot(piece["products"][:, block_len:], piece["value"], 1, 0)
    for piece in pieces:
        right = jnp.concatenate([piece["erase_in"], piece["valued"][:block_len]], axis=1)
        piece["erased"] = split_dot(piece["inverse"], right, 1, 0)
    for piece in pieces:
        read = split_dot(piece["products"][block_len:, :block_len], piece["erased"], 1, 0)
        piece["read_through"] = piece["read_in"] + read[:, :channels]
        piece["read_local"] = read[:, channels:] + piece["valued"][block_len:]
        piece["moved"] = split_dot(piece["erased"], piece["erase_tail"], 0, 0)
        piece["added"] = piece["moved"][channels:] + split_dot(
            piece["value"], piece["key_tail"], 0, 0
        )
    for piece in pieces:
        rows, cut = pl.ds(piece["group"] * block_len, block_len), piece["cut"]
        aug = aug_ref[:, cut]
        out = split_dot(piece["read_through"], aug, 1, 1)
        local_ref[rows, cut] = out[:, :channels] + piece["read_local"]
        through_ref[rows, cut] = out[:, channels:]
        after = aug * piece["total"] + split_dot(aug, piece["moved"][:channels], 1, 0)
        aug_ref[:, cut] = after + jnp.concatenate(
            [piece["added"], jnp.zeros_like(piece["added"])], axis=0
        )

    @pl.when(step == pl.num_programs(0) - 1)
    def _():
        state_ref[...] = aug_ref[...]


def local_scan(fields, channels):
    rows, width = fields[0].shape
    block_len = min(64, rows)
    tile = 2 * block_len if rows % (2 * block_len) == 0 else block_len
    tiled = pl.BlockSpec((tile, width), lambda i: (i, 0))
    return pl.pallas_call(
        functools.partial(scan_kernel, channels, block_len),
        grid=(rows // tile,),
        in_specs=[tiled] * 5,
        out_specs=[tiled, tiled, pl.BlockSpec((2 * channels, width), lambda i: (0, 0))],
        out_shape=[
            jax.ShapeDtypeStruct((rows, width), jnp.float32),
            jax.ShapeDtypeStruct((rows, width), jnp.float32),
            jax.ShapeDtypeStruct((2 * channels, width), jnp.float32),
        ],
        scratch_shapes=[pltpu.VMEM((2 * channels, width), jnp.float32)],
        compiler_params=pltpu.CompilerParams(dimension_semantics=("arbitrary",)),
        cost_estimate=pl.CostEstimate(
            flops=16 * 10**9, bytes_accessed=4 * 10**6, transcendentals=0
        ),
    )(*fields)


def read_kernel(
    channels,
    place_ref,
    states_ref,
    local_ref,
    through_ref,
    r_ref,
    k_ref,
    v_ref,
    own_ref,
    gain_ref,
    weight_ref,
    out_ref,
    enter_ref,
):
    width = local_ref.shape[1]
    cuts = [slice(at, at + channels) for at in range(0, width, channels)]

    @pl.when(pl.program_id(0) == 0)
    def _():
        enter_ref[...] = jnp.zeros_like(enter_ref)

        def one(index, carry):
            for cut in cuts:
                moved = jnp.dot(
                    enter_ref[:, cut],
                    states_ref[index, channels:, cut],
                    precision=precise,
                    preferred_element_type=jnp.float32,
                )
                enter_ref[:, cut] = moved + states_ref[index, :channels, cut]
            return carry

        lax.fori_loop(0, place_ref[0], one, 0)

    through = through_ref[...]
    readout = local_ref[...] + jnp.concatenate(
        [split_dot(through[:, cut], enter_ref[:, cut], 1, 1) for cut in cuts], axis=1
    )
    removed = readout - head_sums(readout, channels) * (1.0 / channels)
    squared = head_sums(removed * removed, channels) * (1.0 / channels)
    own = head_sums(r_ref[...] * k_ref[...] * own_ref[...], channels) * v_ref[...]
    mixed = removed * lax.rsqrt(squared + 0.00064) * gain_ref[...] + own
    out_ref[...] = jnp.dot(
        mixed.astype(jnp.bfloat16), weight_ref[...], preferred_element_type=jnp.float32
    ).astype(jnp.bfloat16)


def read_heads(place, states, local, through, receive, key, value, own, gain, weight, channels):
    rows, width = local.shape
    tile = min(128, rows)
    tiled = pl.BlockSpec((tile, width), lambda i: (i, 0))
    row_of = pl.BlockSpec((1, width), lambda i: (0, 0))
    return pl.pallas_call(
        functools.partial(read_kernel, channels),
        grid=(rows // tile,),
        in_specs=[
            pl.BlockSpec(memory_space=pltpu.SMEM),
            pl.BlockSpec(states.shape, lambda i: (0, 0, 0)),
            tiled,
            tiled,
            tiled,
            tiled,
            tiled,
            row_of,
            row_of,
            pl.BlockSpec(weight.shape, lambda i: (0, 0)),
        ],
        out_specs=pl.BlockSpec((tile, weight.shape[1]), lambda i: (i, 0)),
        out_shape=jax.ShapeDtypeStruct((rows, weight.shape[1]), jnp.bfloat16),
        scratch_shapes=[pltpu.VMEM((channels, width), jnp.float32)],
        compiler_params=pltpu.CompilerParams(dimension_semantics=("arbitrary",)),
        cost_estimate=pl.CostEstimate(
            flops=4 * 10**9, bytes_accessed=8 * 10**6, transcendentals=0
        ),
    )(place, states, local, through, receive, key, value, own, gain, weight)


def per_device(
    mixer_input_rows,
    mixer_norm_scale,
    decay_bias_table,
    erase_bias_table,
    receive_weight,
    key_weight,
    value_weight,
    decay_weight,
    erase_weight,
    self_token_scale,
    head_norm_scale,
    output_weight,
    expert_input_rows,
    expert_norm_scale,
    routes,
    router_weights,
    routed_gate_weight,
    routed_up_weight,
    routed_down_weight,
    common_gate_weight,
    common_up_weight,
    common_down_weight,
):
    normed_b = rms_rows(expert_input_rows, expert_norm_scale)
    route_weight = 2.5 * router_weights / jnp.sum(router_weights, axis=1, keepdims=True)
    token_count, top_count = routes.shape
    expert_count = lax.axis_size("ep") * lax.axis_size("tp")
    capacity = 2 * token_count * top_count // expert_count
    named = [
        routes[:, j : j + 1] == jnp.arange(expert_count, dtype=jnp.int32)[None, :]
        for j in range(top_count)
    ]
    counted = sum(n.astype(jnp.bfloat16) for n in named)
    token = jnp.arange(token_count)
    earlier = (token[:, None] > token[None, :]).astype(jnp.bfloat16)
    ranks = jnp.dot(earlier, counted, preferred_element_type=jnp.float32)
    slots = [
        routes[:, j] * capacity
        + jnp.sum(jnp.where(named[j], ranks, 0.0), axis=1).astype(jnp.int32)
        for j in range(top_count)
    ]
    slot_range = jnp.arange(expert_count * capacity, dtype=jnp.int32)
    chosen_rows = sum((slot_range[:, None] == s[None, :]).astype(jnp.bfloat16) for s in slots)
    outgoing = jnp.dot(chosen_rows, normed_b, preferred_element_type=jnp.float32)
    outgoing = outgoing.astype(jnp.bfloat16).reshape(expert_count, capacity, -1)
    arrived = lax.all_to_all(outgoing, ("ep", "tp"), split_axis=0, concat_axis=0, tiled=True)

    normed_a = rms_rows(mixer_input_rows, mixer_norm_scale)
    row_piece = lax.all_gather(normed_a, "tp", axis=0, tiled=True)
    channels = self_token_scale.shape[1]

    def projected(weight):
        return jnp.dot(row_piece, weight, preferred_element_type=jnp.float32)

    receive = projected(receive_weight)
    key = projected(key_weight)
    value = projected(value_weight)
    decay_in = projected(decay_weight) + jnp.repeat(decay_bias_table, channels, axis=1)
    log_decay = -jnp.exp(-jax.nn.softplus(-decay_in) - 0.5)
    rate = jax.nn.sigmoid(
        projected(erase_weight) + jnp.repeat(erase_bias_table, channels)[None, :]
    )
    local, through, state = local_scan((receive, key, value, log_decay, rate), channels)
    states = lax.all_gather(state, "ep", axis=0, tiled=False)
    partial = read_heads(
        lax.axis_index("ep").astype(jnp.int32).reshape(1),
        states,
        local,
        through,
        receive,
        key,
        value,
        self_token_scale.reshape(1, -1),
        head_norm_scale.reshape(1, -1),
        output_weight,
        channels,
    )
    mixer_output = lax.psum_scatter(partial, "tp", scatter_dimension=0, tiled=True)

    flat_rows = arrived.reshape(-1, arrived.shape[-1])
    expert_hidden = (
        jax.nn.silu(jnp.dot(flat_rows, routed_gate_weight[0], preferred_element_type=jnp.float32))
        * jnp.dot(flat_rows, routed_up_weight[0], preferred_element_type=jnp.float32)
    ).astype(jnp.bfloat16)
    result = jnp.dot(
        expert_hidden, routed_down_weight[0], preferred_element_type=jnp.float32
    ).astype(jnp.bfloat16)
    returned = lax.all_to_all(
        result.reshape(arrived.shape), ("ep", "tp"), split_axis=0, concat_axis=0, tiled=True
    )
    back_rows = returned.reshape(expert_count * capacity, -1)
    combine = sum(
        jnp.where(slots[j][:, None] == slot_range[None, :], route_weight[:, j : j + 1], 0.0)
        for j in range(top_count)
    )
    combine_high = lax.reduce_precision(combine, 8, 7)
    combine_low = combine - combine_high
    routed = jnp.dot(
        combine_high.astype(jnp.bfloat16), back_rows, preferred_element_type=jnp.float32
    ) + jnp.dot(combine_low.astype(jnp.bfloat16), back_rows, preferred_element_type=jnp.float32)
    shared_hidden = (
        jax.nn.silu(jnp.dot(normed_b, common_gate_weight, preferred_element_type=jnp.float32))
        * jnp.dot(normed_b, common_up_weight, preferred_element_type=jnp.float32)
    ).astype(jnp.bfloat16)
    shared_term = jnp.dot(shared_hidden, common_down_weight, preferred_element_type=jnp.float32)
    mixed_b = (routed + shared_term).astype(jnp.bfloat16)
    return (mixer_output, mixed_b)


def solution(mesh):
    in_specs = (
        P(("ep", "tp"), None),
        P(),
        P("ep", "tp"),
        P("tp"),
        P(None, "tp"),
        P(None, "tp"),
        P(None, "tp"),
        P(None, "tp"),
        P(None, "tp"),
        P("tp", None),
        P("tp"),
        P("tp", None),
        P(("ep", "tp"), None),
        P(),
        P(("ep", "tp"), None),
        P(("ep", "tp"), None),
        P(("ep", "tp"), None, None),
        P(("ep", "tp"), None, None),
        P(("ep", "tp"), None, None),
        P(),
        P(),
        P(),
    )
    out_specs = (P(("ep", "tp"), None), P(("ep", "tp"), None))
    return jax.shard_map(
        per_device, mesh=mesh, in_specs=in_specs, out_specs=out_specs, check_vma=False
    )
```

```python
import functools

import jax
import jax.numpy as jnp
from jax import lax
from jax.experimental import pallas as pl
from jax.experimental.pallas import tpu as pltpu
from jax.sharding import PartitionSpec as P

precise = lax.Precision.HIGHEST


def rms_rows(values, feature_gain):
    wide_values = values.astype(jnp.float32)
    inverse = lax.rsqrt(jnp.mean(wide_values * wide_values, axis=1, keepdims=True) + 1e-06)
    return (wide_values * inverse * feature_gain).astype(jnp.bfloat16)


def gathered(block, axis):
    peers = lax.axis_size(axis)
    if peers & (peers - 1):
        return lax.all_gather(block, axis, axis=0, tiled=True)
    place = lax.axis_index(axis)
    held = block[None]
    bit = peers // 2
    while bit:
        other = lax.ppermute(held, axis, [(i, i ^ bit) for i in range(peers)])
        upper = (place & bit) != 0
        low, high = jnp.where(upper, other, held), jnp.where(upper, held, other)
        held = jnp.stack([low, high], axis=0).reshape((2 * held.shape[0],) + block.shape)
        bit //= 2
    bits = peers.bit_length() - 1
    order = [sum(((i >> b) & 1) << (bits - 1 - b) for b in range(bits)) for i in range(peers)]
    return jnp.concatenate([held[i] for i in order], axis=0)


def halves(wide):
    high = wide.astype(jnp.bfloat16)
    return high, (wide - high.astype(jnp.float32)).astype(jnp.bfloat16)


def split_dot(left, right, left_axis, right_axis):
    left_high, left_low = halves(left)
    right_high, right_low = halves(right)
    return lax.dot_general(
        jnp.concatenate([left_high, left_high, left_low], axis=left_axis),
        jnp.concatenate([right_high, right_low, right_high], axis=right_axis),
        (((left_axis,), (right_axis,)), ((), ())),
        preferred_element_type=jnp.float32,
    )


def head_sums(wide, channels):
    rows, width = wide.shape
    same_head = (
        lax.broadcasted_iota(jnp.int32, (width, width), 0) // channels
        == lax.broadcasted_iota(jnp.int32, (width, width), 1) // channels
    )
    ones = jnp.where(same_head, 1.0, 0.0).astype(jnp.bfloat16)
    high, low = halves(wide)
    both = jnp.dot(
        jnp.concatenate([high, low], axis=0), ones, preferred_element_type=jnp.float32
    )
    return both[:rows] + both[rows:]


def scan_kernel(
    channels, block_len, r_ref, k_ref, v_ref, ld_ref, rate_ref, local_ref, through_ref, state_ref, aug_ref
):
    step = pl.program_id(0)
    width = r_ref.shape[1]
    heads = width // channels
    groups = r_ref.shape[0] // block_len

    def iotas(shape):
        return (
            lax.broadcasted_iota(jnp.int32, shape, 0),
            lax.broadcasted_iota(jnp.int32, shape, 1),
        )

    row, col = iotas((block_len, block_len))
    eye = jnp.where(row == col, 1.0, 0.0)
    wide_row, wide_col = iotas((2 * block_len, 2 * block_len))
    local_row, local_col = wide_row % block_len, wide_col % block_len
    keep = (local_row > local_col) | ((local_row == local_col) & (wide_row >= block_len))
    tri_row, tri_col = iotas((block_len, 3 * block_len))
    running = jnp.where(tri_row >= tri_col % block_len, 1.0, 0.0).astype(jnp.bfloat16)

    @pl.when(step == 0)
    def _():
        aug_row, aug_col = iotas((2 * channels, width))
        aug_ref[...] = jnp.where(aug_row - channels == aug_col % channels, 1.0, 0.0)

    pieces = []
    for group in range(groups):
        rows = pl.ds(group * block_len, block_len)
        receive, key, value = r_ref[rows, :], k_ref[rows, :], v_ref[rows, :]
        log_decay, rate = ld_ref[rows, :], rate_ref[rows, :]
        unit = key * lax.rsqrt(head_sums(key * key, channels) + 1e-06)
        high, rest = halves(log_decay)
        middle, low = halves(log_decay - high.astype(jnp.float32))
        cumulative = jnp.dot(
            running,
            jnp.concatenate([high, middle, low], axis=0),
            preferred_element_type=jnp.float32,
        )
        growth = jnp.exp(-cumulative)
        erase_in = -unit * jnp.exp(cumulative - log_decay)
        erase_out = unit * rate * growth
        key_out = key * growth
        read_in = receive * jnp.exp(cumulative)
        last = cumulative[block_len - 1 : block_len, :]
        tail = jnp.exp(last - cumulative)
        erase_tail = unit * rate * tail
        key_tail = key * tail
        total = jnp.exp(last)
        for head in range(heads):
            cut = slice(head * channels, (head + 1) * channels)
            products = split_dot(
                jnp.concatenate([erase_in[:, cut], read_in[:, cut]], axis=0),
                jnp.concatenate([erase_out[:, cut], key_out[:, cut]], axis=0),
                1,
                1,
            )
            products = jnp.where(keep, products, 0.0)
            pieces.append(
                dict(
                    group=group,
                    cut=cut,
                    products=products,
                    erase_in=erase_in[:, cut],
                    read_in=read_in[:, cut],
                    value=value[:, cut],
                    erase_tail=erase_tail[:, cut],
                    key_tail=key_tail[:, cut],
                    total=total[:, cut],
                    erase=products[:block_len, :block_len],
                )
            )
    for piece in pieces:
        piece["inverse"] = eye + jnp.where(row // 2 == col // 2, piece["erase"], 0.0)
    span = 2
    while span < block_len:
        joint = (row // (2 * span) == col // (2 * span)) & (row // span != col // span)
        for piece in pieces:
            piece["half"] = split_dot(piece["inverse"], jnp.where(joint, piece["erase"], 0.0), 1, 0)
        for piece in pieces:
            piece["inverse"] = piece["inverse"] + split_dot(piece["half"], piece["inverse"], 1, 0)
        span *= 2
    for piece in pieces:
        piece["valued"] = split_dot(piece["products"][:, block_len:], piece["value"], 1, 0)
    for piece in pieces:
        right = jnp.concatenate([piece["erase_in"], piece["valued"][:block_len]], axis=1)
        piece["erased"] = split_dot(piece["inverse"], right, 1, 0)
    for piece in pieces:
        read = split_dot(piece["products"][block_len:, :block_len], piece["erased"], 1, 0)
        piece["read_through"] = piece["read_in"] + read[:, :channels]
        piece["read_local"] = read[:, channels:] + piece["valued"][block_len:]
        piece["moved"] = split_dot(piece["erased"], piece["erase_tail"], 0, 0)
        piece["added"] = piece["moved"][channels:] + split_dot(
            piece["value"], piece["key_tail"], 0, 0
        )
    for piece in pieces:
        rows, cut = pl.ds(piece["group"] * block_len, block_len), piece["cut"]
        aug = aug_ref[:, cut]
        out = split_dot(piece["read_through"], aug, 1, 1)
        local_ref[rows, cut] = out[:, :channels] + piece["read_local"]
        through_ref[rows, cut] = out[:, channels:]
        after = aug * piece["total"] + split_dot(aug, piece["moved"][:channels], 1, 0)
        aug_ref[:, cut] = after + jnp.concatenate(
            [piece["added"], jnp.zeros_like(piece["added"])], axis=0
        )

    @pl.when(step == pl.num_programs(0) - 1)
    def _():
        state_ref[...] = aug_ref[...]


def local_scan(fields, channels):
    rows, width = fields[0].shape
    block_len = min(64, rows)
    tile = 2 * block_len if rows % (2 * block_len) == 0 else block_len
    tiled = pl.BlockSpec((tile, width), lambda i: (i, 0))
    return pl.pallas_call(
        functools.partial(scan_kernel, channels, block_len),
        grid=(rows // tile,),
        in_specs=[tiled] * 5,
        out_specs=[tiled, tiled, pl.BlockSpec((2 * channels, width), lambda i: (0, 0))],
        out_shape=[
            jax.ShapeDtypeStruct((rows, width), jnp.float32),
            jax.ShapeDtypeStruct((rows, width), jnp.float32),
            jax.ShapeDtypeStruct((2 * channels, width), jnp.float32),
        ],
        scratch_shapes=[pltpu.VMEM((2 * channels, width), jnp.float32)],
        compiler_params=pltpu.CompilerParams(dimension_semantics=("arbitrary",)),
        cost_estimate=pl.CostEstimate(
            flops=16 * 10**9, bytes_accessed=4 * 10**6, transcendentals=0
        ),
    )(*fields)


def read_kernel(
    channels,
    place_ref,
    states_ref,
    local_ref,
    through_ref,
    r_ref,
    k_ref,
    v_ref,
    own_ref,
    gain_ref,
    weight_ref,
    out_ref,
    enter_ref,
):
    width = local_ref.shape[1]
    cuts = [slice(at, at + channels) for at in range(0, width, channels)]

    @pl.when(pl.program_id(0) == 0)
    def _():
        enter_ref[...] = jnp.zeros_like(enter_ref)

        def one(index, carry):
            for cut in cuts:
                moved = jnp.dot(
                    enter_ref[:, cut],
                    states_ref[index, channels:, cut],
                    precision=precise,
                    preferred_element_type=jnp.float32,
                )
                enter_ref[:, cut] = moved + states_ref[index, :channels, cut]
            return carry

        lax.fori_loop(0, place_ref[0], one, 0)

    through = through_ref[...]
    readout = local_ref[...] + jnp.concatenate(
        [split_dot(through[:, cut], enter_ref[:, cut], 1, 1) for cut in cuts], axis=1
    )
    removed = readout - head_sums(readout, channels) * (1.0 / channels)
    squared = head_sums(removed * removed, channels) * (1.0 / channels)
    own = head_sums(r_ref[...] * k_ref[...] * own_ref[...], channels) * v_ref[...]
    mixed = removed * lax.rsqrt(squared + 0.00064) * gain_ref[...] + own
    out_ref[...] = jnp.dot(
        mixed.astype(jnp.bfloat16), weight_ref[...], preferred_element_type=jnp.float32
    ).astype(jnp.bfloat16)


def read_heads(place, states, local, through, receive, key, value, own, gain, weight, channels):
    rows, width = local.shape
    tile = min(128, rows)
    tiled = pl.BlockSpec((tile, width), lambda i: (i, 0))
    row_of = pl.BlockSpec((1, width), lambda i: (0, 0))
    return pl.pallas_call(
        functools.partial(read_kernel, channels),
        grid=(rows // tile,),
        in_specs=[
            pl.BlockSpec(memory_space=pltpu.SMEM),
            pl.BlockSpec(states.shape, lambda i: (0, 0, 0)),
            tiled,
            tiled,
            tiled,
            tiled,
            tiled,
            row_of,
            row_of,
            pl.BlockSpec(weight.shape, lambda i: (0, 0)),
        ],
        out_specs=pl.BlockSpec((tile, weight.shape[1]), lambda i: (i, 0)),
        out_shape=jax.ShapeDtypeStruct((rows, weight.shape[1]), jnp.bfloat16),
        scratch_shapes=[pltpu.VMEM((channels, width), jnp.float32)],
        compiler_params=pltpu.CompilerParams(dimension_semantics=("arbitrary",)),
        cost_estimate=pl.CostEstimate(
            flops=4 * 10**9, bytes_accessed=8 * 10**6, transcendentals=0
        ),
    )(place, states, local, through, receive, key, value, own, gain, weight)


def per_device(
    mixer_input_rows,
    mixer_norm_scale,
    decay_bias_table,
    erase_bias_table,
    receive_weight,
    key_weight,
    value_weight,
    decay_weight,
    erase_weight,
    self_token_scale,
    head_norm_scale,
    output_weight,
    expert_input_rows,
    expert_norm_scale,
    routes,
    router_weights,
    routed_gate_weight,
    routed_up_weight,
    routed_down_weight,
    common_gate_weight,
    common_up_weight,
    common_down_weight,
):
    normed_b = rms_rows(expert_input_rows, expert_norm_scale)
    route_weight = 2.5 * router_weights / jnp.sum(router_weights, axis=1, keepdims=True)
    token_count, top_count = routes.shape
    expert_count = lax.axis_size("ep") * lax.axis_size("tp")
    capacity = 2 * token_count * top_count // expert_count
    named = [
        routes[:, j : j + 1] == jnp.arange(expert_count, dtype=jnp.int32)[None, :]
        for j in range(top_count)
    ]
    counted = sum(n.astype(jnp.bfloat16) for n in named)
    token = jnp.arange(token_count)
    earlier = (token[:, None] > token[None, :]).astype(jnp.bfloat16)
    ranks = jnp.dot(earlier, counted, preferred_element_type=jnp.float32)
    slots = [
        routes[:, j] * capacity
        + jnp.sum(jnp.where(named[j], ranks, 0.0), axis=1).astype(jnp.int32)
        for j in range(top_count)
    ]
    slot_range = jnp.arange(expert_count * capacity, dtype=jnp.int32)
    chosen_rows = sum((slot_range[:, None] == s[None, :]).astype(jnp.bfloat16) for s in slots)
    outgoing = jnp.dot(chosen_rows, normed_b, preferred_element_type=jnp.float32)
    outgoing = outgoing.astype(jnp.bfloat16).reshape(expert_count, capacity, -1)
    arrived = lax.all_to_all(outgoing, ("ep", "tp"), split_axis=0, concat_axis=0, tiled=True)

    normed_a = rms_rows(mixer_input_rows, mixer_norm_scale)
    row_piece = gathered(normed_a, "tp")
    channels = self_token_scale.shape[1]

    def projected(weight):
        return jnp.dot(row_piece, weight, preferred_element_type=jnp.float32)

    receive = projected(receive_weight)
    key = projected(key_weight)
    value = projected(value_weight)
    decay_in = projected(decay_weight) + jnp.repeat(decay_bias_table, channels, axis=1)
    log_decay = -jnp.exp(-jax.nn.softplus(-decay_in) - 0.5)
    rate = jax.nn.sigmoid(
        projected(erase_weight) + jnp.repeat(erase_bias_table, channels)[None, :]
    )
    local, through, state = local_scan((receive, key, value, log_decay, rate), channels)
    states = lax.all_gather(state, "ep", axis=0, tiled=False)
    partial = read_heads(
        lax.axis_index("ep").astype(jnp.int32).reshape(1),
        states,
        local,
        through,
        receive,
        key,
        value,
        self_token_scale.reshape(1, -1),
        head_norm_scale.reshape(1, -1),
        output_weight,
        channels,
    )
    mixer_output = lax.psum_scatter(partial, "tp", scatter_dimension=0, tiled=True)

    flat_rows = arrived.reshape(-1, arrived.shape[-1])
    expert_hidden = (
        jax.nn.silu(jnp.dot(flat_rows, routed_gate_weight[0], preferred_element_type=jnp.float32))
        * jnp.dot(flat_rows, routed_up_weight[0], preferred_element_type=jnp.float32)
    ).astype(jnp.bfloat16)
    result = jnp.dot(
        expert_hidden, routed_down_weight[0], preferred_element_type=jnp.float32
    ).astype(jnp.bfloat16)
    returned = lax.all_to_all(
        result.reshape(arrived.shape), ("ep", "tp"), split_axis=0, concat_axis=0, tiled=True
    )
    back_rows = returned.reshape(expert_count * capacity, -1)
    combine = sum(
        jnp.where(slots[j][:, None] == slot_range[None, :], route_weight[:, j : j + 1], 0.0)
        for j in range(top_count)
    )
    combine_high = lax.reduce_precision(combine, 8, 7)
    combine_low = combine - combine_high
    routed = jnp.dot(
        combine_high.astype(jnp.bfloat16), back_rows, preferred_element_type=jnp.float32
    ) + jnp.dot(combine_low.astype(jnp.bfloat16), back_rows, preferred_element_type=jnp.float32)
    shared_hidden = (
        jax.nn.silu(jnp.dot(normed_b, common_gate_weight, preferred_element_type=jnp.float32))
        * jnp.dot(normed_b, common_up_weight, preferred_element_type=jnp.float32)
    ).astype(jnp.bfloat16)
    shared_term = jnp.dot(shared_hidden, common_down_weight, preferred_element_type=jnp.float32)
    mixed_b = (routed + shared_term).astype(jnp.bfloat16)
    return (mixer_output, mixed_b)


def solution(mesh):
    in_specs = (
        P(("ep", "tp"), None),
        P(),
        P("ep", "tp"),
        P("tp"),
        P(None, "tp"),
        P(None, "tp"),
        P(None, "tp"),
        P(None, "tp"),
        P(None, "tp"),
        P("tp", None),
        P("tp"),
        P("tp", None),
        P(("ep", "tp"), None),
        P(),
        P(("ep", "tp"), None),
        P(("ep", "tp"), None),
        P(("ep", "tp"), None, None),
        P(("ep", "tp"), None, None),
        P(("ep", "tp"), None, None),
        P(),
        P(),
        P(),
    )
    out_specs = (P(("ep", "tp"), None), P(("ep", "tp"), None))
    return jax.shard_map(
        per_device, mesh=mesh, in_specs=in_specs, out_specs=out_specs, check_vma=False
    )
```
